32 devices in a mesh: sp: 16 (over z, y, x), tp: 2 (over core).
Axes of the slice: x: 2, y: 2, z: 4, core: 2. Of those that a mesh axis runs over, the one named last changes fastest.
Arguments:
- residual_in: bfloat16 [4096, 2048], P(('sp', 'tp')), may hold values from -6 to 6
- query_lean: bfloat16 [4096, 8, 96], P('sp', 'tp'), may hold values from -60 to 60
- query_broad: bfloat16 [4096, 8, 160], P('sp', 'tp'), may hold values from -60 to 60
- latent: bfloat16 [4096, 256], P('sp'), may hold values from -6 to 6
- rope_key: bfloat16 [4096, 32], P('sp'), may hold values from -8 to 8
- latent_gain: float32 [256], replicated, may hold values from 0.1 to 1.9
- key_up_lean: bfloat16 [256, 8, 64], P(None, 'tp'), may hold values from -0.375 to 0.375
- key_up_broad: bfloat16 [256, 8, 128], P(None, 'tp'), may hold values from -0.375 to 0.375
- value_up_lean: bfloat16 [256, 8, 64], P(None, 'tp'), may hold values from -0.375 to 0.375
- value_up_broad: bfloat16 [256, 8, 128], P(None, 'tp'), may hold values from -0.375 to 0.375
- out_lean: bfloat16 [8, 64, 2048], P('tp'), may hold values from -0.15625 to 0.15625
- out_broad: bfloat16 [8, 128, 2048], P('tp'), may hold values from -0.15625 to 0.15625
- attn_gain: float32 [2048], replicated, may hold values from 0.1 to 1.9
- mlp_gain: float32 [2048], replicated, may hold values from 0.1 to 1.9
- gate_weight: bfloat16 [2048, 2816], P('sp', 'tp'), may hold values from -0.125 to 0.125
- up_weight: bfloat16 [2048, 2816], P('sp', 'tp'), may hold values from -0.125 to 0.125
- down_weight: bfloat16 [2816, 2048], P('tp', 'sp'), may hold values from -0.109375 to 0.109375
Outputs:
- layer_out: bfloat16 [4096, 2048], P(('sp', 'tp'))
The draws below stay inside these ranges and needn't reach their ends.
All inputs are finite; a program needn't handle non-finite values.
Results may differ from the reference program's by a relative error of at most 0.015.
Values may be sent and summed in bfloat16 or wider, within the bound.
No kernel may reach another device: no remote copies, remote signals or barrier semaphores. Data moves between devices by JAX's collectives and lax.ppermute only.
A program may use at most 128 MiB of HBM per device.

```python
import math
import jax
import jax.numpy as jnp
from jax import lax

D = 2048
HEADS_A = 8
HEADS_B = 8
NOPE_A = 64
V_A = 64
NOPE_B = 128
V_B = 128
ROPE = 32
KV_RANK = 256
FF = 2816
QK_A = 96
QK_B = 160
TOKENS = 4096
N_TP = 2


def draw_rope_key(key, part):
    base = jax.random.truncated_normal(jax.random.fold_in(key, 1), -4.0, 4.0, (TOKENS, ROPE), jnp.float32)
    return base.astype(jnp.bfloat16)


def draw_query_lean(key, part):
    base = jax.random.truncated_normal(jax.random.fold_in(key, 2), -4.0, 4.0, (TOKENS, HEADS_A, QK_A), jnp.float32)
    return base.astype(jnp.bfloat16)


def draw_query_broad(key, part):
    base = jax.random.truncated_normal(jax.random.fold_in(key, 3), -4.0, 4.0, (TOKENS, HEADS_B, QK_B), jnp.float32)
    return base.astype(jnp.bfloat16)


def levels(key, extent, pieces, smallest, high):
    def one(position, shards_of):
        heights = jax.random.uniform(jax.random.fold_in(jax.random.fold_in(key, 6), position), (shards_of,), jnp.float32, smallest / len(pieces), high / len(pieces))
        return jnp.repeat(jnp.exp(heights), extent[position] // shards_of).reshape((-1,) + (1,) * (len(extent) - position - 1))

    factor_of = one(*pieces[0])
    for cut in pieces[1:]:
        factor_of = factor_of * one(*cut)
    return factor_of


def centred(own_key, extent, scale, bound, cuts=(), held_as=jnp.bfloat16):
    loudness = levels(own_key, extent, cuts, -0.22, 0.18) if cuts else 1.0
    values = jax.random.normal(own_key, extent, jnp.float32) * scale * loudness
    return jnp.minimum(jnp.maximum(values, -bound), bound).astype(held_as)


def setup_inputs(seed: int = 0) -> dict:
    seeds = jax.random.split(jax.random.key(seed), 18)
    return {
        "residual_in": centred(seeds[0], (TOKENS, D), 1.0, 6.0, ((0, 32),)),
        "query_lean": draw_query_lean(jax.random.fold_in(seeds[17], 71), 0),
        "query_broad": draw_query_broad(jax.random.fold_in(seeds[17], 71), 0),
        "latent": centred(seeds[3], (TOKENS, KV_RANK), 1.0, 6.0, ((0, 16),)),
        "rope_key": draw_rope_key(jax.random.fold_in(seeds[17], 71), 0),
        "latent_gain": jnp.clip(1.0 + 0.18 * jax.random.normal(seeds[5], (KV_RANK,), jnp.float32), 0.1, 1.9),
        "key_up_lean": centred(seeds[6], (KV_RANK, HEADS_A, NOPE_A), KV_RANK ** -0.5, 0.375, ((1, 2),)),
        "key_up_broad": centred(seeds[7], (KV_RANK, HEADS_B, NOPE_B), KV_RANK ** -0.5, 0.375, ((1, 2),)),
        "value_up_lean": centred(seeds[8], (KV_RANK, HEADS_A, V_A), KV_RANK ** -0.5, 0.375, ((1, 2),)),
        "value_up_broad": centred(seeds[9], (KV_RANK, HEADS_B, V_B), KV_RANK ** -0.5, 0.375, ((1, 2),)),
        "out_lean": centred(seeds[10], (HEADS_A, V_A, D), (HEADS_A * V_A + HEADS_B * V_B) ** -0.5, 0.15625, ((0, 2),)),
        "out_broad": centred(seeds[11], (HEADS_B, V_B, D), (HEADS_A * V_A + HEADS_B * V_B) ** -0.5, 0.15625, ((0, 2),)),
        "attn_gain": jnp.clip(1.0 + 0.18 * jax.random.normal(seeds[12], (D,), jnp.float32), 0.1, 1.9),
        "mlp_gain": jnp.clip(1.0 + 0.18 * jax.random.normal(seeds[13], (D,), jnp.float32), 0.1, 1.9),
        "gate_weight": centred(seeds[14], (D, FF), D ** -0.5, 0.125, ((0, 16), (1, 2))),
        "up_weight": centred(seeds[15], (D, FF), D ** -0.5, 0.125, ((0, 16), (1, 2))),
        "down_weight": centred(seeds[16], (FF, D), FF ** -0.5, 0.109375, ((0, 2), (1, 16))),
    }


THETA = 10000.0
EPS = 1e-06
NEGATIVE = -1e+30

def rotate(values, positions):
    width = values.shape[-1]
    half = width // 2
    freqs = THETA ** (-2.0 * jnp.arange(half, dtype=jnp.float32) / width)
    angle = positions.astype(jnp.float32)[:, None] * freqs[None, :]
    cosine = jnp.cos(angle)
    sine = jnp.sin(angle)
    if values.ndim == 3:
        cosine = cosine[:, None, :]
        sine = sine[:, None, :]
    first = values[..., :half]
    second = values[..., half:]
    return jnp.concatenate([first * cosine - second * sine, first * sine + second * cosine], axis=-1)

def normalize(values, gain):
    return values * lax.rsqrt(lax.optimization_barrier(jnp.mean(values * values, axis=-1, keepdims=True)) + EPS) * gain.astype(jnp.float32)

def widen(values):
    return lax.optimization_barrier(values).astype(jnp.float32)

def attend_group(query, key_up, value_up, latent_normed, rotated_key, positions):
    nope = key_up.shape[2]
    heads = key_up.shape[1]
    vsize = value_up.shape[2]
    scale = query.shape[2] ** (-0.5)
    lat = latent_normed.astype(jnp.float32)
    keys = widen(jnp.einsum('kr,rhd->khd', lat, key_up.astype(jnp.float32)).astype(jnp.bfloat16))
    values = widen(jnp.einsum('kr,rhd->khd', lat, value_up.astype(jnp.float32)).astype(jnp.bfloat16))
    rot_keys = rotated_key.astype(jnp.float32)
    query_nope = query[:, :, :nope].astype(jnp.float32)
    query_rot = widen(rotate(query[:, :, nope:].astype(jnp.float32), positions).astype(jnp.bfloat16))
    size = math.gcd(TOKENS, 256)

    def block(index):
        start = (index * size).astype(jnp.int32)
        rows = start + jnp.arange(size, dtype=jnp.int32)
        part_nope = lax.dynamic_slice_in_dim(query_nope, start, size, 0)
        part_rot = lax.dynamic_slice_in_dim(query_rot, start, size, 0)
        scores = (jnp.einsum('qhd,khd->hqk', part_nope, keys) + jnp.einsum('qhr,kr->hqk', part_rot, rot_keys)) * scale
        visible = positions[None, :] <= rows[:, None]
        scores = jnp.where(visible[None], scores, NEGATIVE)
        peak = lax.optimization_barrier(jnp.max(scores, axis=-1, keepdims=True))
        weights = jnp.where(visible[None], jnp.exp(scores - peak), 0.0)
        total = lax.optimization_barrier(jnp.sum(weights, axis=-1))
        rounded = widen(weights.astype(jnp.bfloat16))
        result = jnp.einsum('hqk,khv->qhv', rounded, values) / jnp.transpose(total)[:, :, None]
        return result.astype(jnp.bfloat16)
    blocks = lax.map(block, jnp.arange(TOKENS // size, dtype=jnp.int32))
    return blocks.reshape(TOKENS, heads, vsize)

def reference(residual_in, query_lean, query_broad, latent, rope_key, latent_gain, key_up_lean, key_up_broad, value_up_lean, value_up_broad, out_lean, out_broad, attn_gain, mlp_gain, gate_weight, up_weight, down_weight):
    positions = jnp.arange(TOKENS, dtype=jnp.int32)
    latent_normed = normalize(latent.astype(jnp.float32), latent_gain).astype(jnp.bfloat16)
    rotated_key = rotate(rope_key.astype(jnp.float32), positions).astype(jnp.bfloat16)
    attended_lean = attend_group(query_lean, key_up_lean, value_up_lean, latent_normed, rotated_key, positions)
    attended_broad = attend_group(query_broad, key_up_broad, value_up_broad, latent_normed, rotated_key, positions)
    lean_per = HEADS_A // N_TP
    broad_per = HEADS_B // N_TP
    head_sum = jnp.zeros((TOKENS, D), jnp.float32)
    for group in range(N_TP):
        partial_value = jnp.einsum('qhv,hvd->qd', attended_lean[:, group * lean_per:(group + 1) * lean_per].astype(jnp.float32), out_lean[group * lean_per:(group + 1) * lean_per].astype(jnp.float32))
        partial_value = partial_value + jnp.einsum('qhv,hvd->qd', attended_broad[:, group * broad_per:(group + 1) * broad_per].astype(jnp.float32), out_broad[group * broad_per:(group + 1) * broad_per].astype(jnp.float32))
        head_sum = head_sum + partial_value.astype(jnp.bfloat16).astype(jnp.float32)
    branch = normalize(head_sum, attn_gain)
    mixed = (residual_in.astype(jnp.float32) + branch).astype(jnp.bfloat16)
    normed = normalize(mixed.astype(jnp.float32), mlp_gain).astype(jnp.bfloat16)
    gate = jnp.dot(normed, gate_weight, preferred_element_type=jnp.float32)
    up = jnp.dot(normed, up_weight, preferred_element_type=jnp.float32)
    hidden = (jax.nn.silu(gate) * up).astype(jnp.bfloat16)
    units = FF // N_TP
    channel_sum = jnp.zeros((TOKENS, D), jnp.float32)
    for group in range(N_TP):
        partial_value = jnp.dot(hidden[:, group * units:(group + 1) * units], down_weight[group * units:(group + 1) * units], preferred_element_type=jnp.float32)
        channel_sum = channel_sum + partial_value.astype(jnp.bfloat16).astype(jnp.float32)
    return (mixed.astype(jnp.float32) + 0.5 * channel_sum).astype(jnp.bfloat16)
```

```python
import functools
import math

import jax
import jax.numpy as jnp
from jax import lax
from jax.experimental import pallas as pl
from jax.experimental.pallas import tpu as pltpu
from jax.sharding import PartitionSpec as P

THETA = 10000.0
EPS = 1e-06
NEGATIVE = -1e30
LOG2E = math.log2(math.e)
BF = jnp.bfloat16
F32 = jnp.float32


def rotate(values, positions):
    width = values.shape[-1]
    half = width // 2
    freqs = THETA ** (-2.0 * jnp.arange(half, dtype=F32) / width)
    angle = positions.astype(F32)[:, None] * freqs[None, :]
    cosine = jnp.cos(angle)
    sine = jnp.sin(angle)
    if values.ndim == 3:
        cosine = cosine[:, None, :]
        sine = sine[:, None, :]
    first = values[..., :half]
    second = values[..., half:]
    return jnp.concatenate(
        [first * cosine - second * sine, first * sine + second * cosine], axis=-1
    )


def normalize(values, gain):
    return values * lax.rsqrt(jnp.mean(values * values, axis=-1, keepdims=True) + EPS) * gain


def attention_kernel(count_ref, q_ref, k_ref, qpos_ref, kpos_ref, o_ref, m_ref, l_ref, acc_ref, *, block, own, rank):
    heads, rows, _ = q_ref.shape

    def step(start, masked, init):
        keys = k_ref[pl.ds(start, block), :]
        latent = keys[:, :rank]
        if masked:
            visible = kpos_ref[:, pl.ds(start, block)] <= qpos_ref[:, :1]
        for h in range(heads):
            scores = lax.dot_general(
                q_ref[h], keys, (((1,), (1,)), ((), ())), preferred_element_type=F32
            )
            if masked:
                scores = jnp.where(visible, scores, NEGATIVE)
            top = jnp.max(scores, axis=1, keepdims=True)
            if init:
                peak = top
            else:
                old = m_ref[h][:, :1]
                peak = jnp.maximum(old, top)
                factor = jnp.exp2(old - peak)
            weights = jnp.exp2(scores - peak)
            part = weights[:, :128]
            for c in range(1, block // 128):
                part = part + weights[:, c * 128 : (c + 1) * 128]
            moved = jnp.dot(weights.astype(BF), latent, preferred_element_type=F32)
            m_ref[h] = jnp.broadcast_to(peak, (rows, 128))
            if init:
                l_ref[h] = part
                acc_ref[h] = moved
            else:
                l_ref[h] = l_ref[h] * factor + part
                acc_ref[h] = acc_ref[h] * factor + moved

    step(0, True, True)
    for b in range(1, own // block):
        step(b * block, True, False)

    def body(i, carry):
        step(pl.multiple_of(i * block, block), False, False)
        return carry

    lax.fori_loop(own // block, count_ref[0], body, 0)
    for h in range(heads):
        total = jnp.sum(l_ref[h], axis=1, keepdims=True)
        o_ref[h] = (acc_ref[h] / total).astype(BF)


def attention(count, q, keys, qpos, kpos, own, rank):
    heads, rows, _ = q.shape
    block = math.gcd(own, 512)
    vmem = pl.BlockSpec(memory_space=pltpu.VMEM)
    return pl.pallas_call(
        functools.partial(attention_kernel, block=block, own=own, rank=rank),
        out_shape=jax.ShapeDtypeStruct((heads, rows, rank), BF),
        in_specs=[pl.BlockSpec(memory_space=pltpu.SMEM), vmem, vmem, vmem, vmem],
        out_specs=vmem,
        scratch_shapes=[
            pltpu.VMEM((heads, rows, 128), F32),
            pltpu.VMEM((heads, rows, 128), F32),
            pltpu.VMEM((heads, rows, rank), F32),
        ],
        cost_estimate=pl.CostEstimate(
            flops=40_000_000_000, transcendentals=heads * rows * keys.shape[0], bytes_accessed=8_000_000
        ),
        name="attn",
    )(count * (own // block), q, keys, qpos, kpos)


def ffn_kernel(order_ref, x_ref, gu_ref, d_ref, o_ref, g_s, u_s, d_s, *, rows):
    chunks = gu_ref.shape[0]
    wide = gu_ref.shape[3]
    for c in range(chunks):
        at = pl.multiple_of(order_ref[c] * wide, wide)
        g_s[:, pl.ds(at, wide)] = gu_ref[c, 0]
        u_s[:, pl.ds(at, wide)] = gu_ref[c, 1]
        d_s[:, pl.ds(at, wide)] = d_ref[c, 0]
    contract = (((1,), (1,)), ((), ()))
    for i in range(x_ref.shape[0] // rows):
        x = x_ref[i * rows : (i + 1) * rows, :]
        gate = lax.dot_general(x, g_s[...], contract, preferred_element_type=F32)
        up = lax.dot_general(x, u_s[...], contract, preferred_element_type=F32)
        hidden = (gate / (1.0 + jnp.exp(-gate)) * up).astype(BF)
        o_ref[i * rows : (i + 1) * rows, :] = jnp.dot(
            hidden, d_s[...], preferred_element_type=F32
        ).astype(BF)


def ffn(order, x, gu, down):
    vmem = pl.BlockSpec(memory_space=pltpu.VMEM)
    tokens, width = x.shape
    hidden = gu.shape[2]
    scratch = pltpu.VMEM((hidden, width), BF)
    return pl.pallas_call(
        functools.partial(ffn_kernel, rows=math.gcd(tokens, 256)),
        out_shape=jax.ShapeDtypeStruct((tokens, width), BF),
        in_specs=[pl.BlockSpec(memory_space=pltpu.SMEM), vmem, vmem, vmem],
        out_specs=vmem,
        scratch_shapes=[scratch, scratch, scratch],
        cost_estimate=pl.CostEstimate(
            flops=6 * tokens * width * hidden, transcendentals=tokens * hidden, bytes_accessed=12_000_000
        ),
        name="ffn",
    )(order, x, gu, down)


def shards(
    residual_in,
    query_lean,
    query_broad,
    latent,
    rope_key,
    latent_gain,
    key_up_lean,
    key_up_broad,
    value_up_lean,
    value_up_broad,
    out_lean,
    out_broad,
    attn_gain,
    mlp_gain,
    gate_weight,
    up_weight,
    down_weight,
):
    here = query_lean.shape[0]
    n_tp = lax.axis_size("tp")
    n_sp = lax.axis_size("sp")
    group = math.gcd(n_sp, 4)
    ranks = n_sp // group
    share = here // n_tp
    s = lax.axis_index("sp")
    t = lax.axis_index("tp")
    g = s % group
    r = s // group
    width = rope_key.shape[1]
    rank = latent.shape[1]

    def over_tp(x, k):
        return lax.ppermute(x, "tp", [(i, (i + k) % n_tp) for i in range(n_tp)])

    def over_group(x, j):
        return lax.ppermute(x, "sp", [(i, i ^ j) for i in range(n_sp)])

    def cut(x, index, size):
        return lax.dynamic_slice_in_dim(x, index * size, size, 0)

    lat_rows = cut(latent, t, share).astype(F32)
    rope_rows = cut(rope_key, t, share).astype(F32)
    row_pos = s * here + t * share + jnp.arange(share, dtype=jnp.int32)
    mine = jnp.concatenate(
        [normalize(lat_rows, latent_gain).astype(BF), rotate(rope_rows, row_pos).astype(BF)], axis=1
    )
    column = [mine] + [
        lax.ppermute(mine, "sp", [(i, i + group * k) for i in range(n_sp - group * k)])
        for k in range(1, ranks)
    ]
    column = jnp.stack(column)
    square = jnp.stack([column] + [over_group(column, j) for j in range(1, group)], axis=1)
    keys = jnp.stack([square] + [over_tp(square, k) for k in range(1, n_tp)], axis=2)
    keys = keys.reshape(ranks * group * here, rank + width)
    own = group * here
    kpos = (
        ((r * group + (g ^ jnp.arange(group))) * here)[:, None, None]
        + (((t - jnp.arange(n_tp)) % n_tp) * share)[None, :, None]
        + jnp.arange(share)[None, None, :]
    ).reshape(1, own).astype(jnp.int32)
    qpos = s * here + jnp.arange(here, dtype=jnp.int32)

    hidden = gate_weight.shape[1] // group
    w_gu = jnp.stack([gate_weight.T, up_weight.T]).reshape(2, group, hidden, -1).swapaxes(0, 1)
    w_d = down_weight.reshape(group, 1, hidden, -1)

    def spread(w):
        pieces = [lax.dynamic_index_in_dim(w, g, 0, keepdims=False)]
        for j in range(1, group):
            pieces.append(over_group(lax.dynamic_index_in_dim(w, g ^ j, 0, keepdims=False), j))
        return jnp.stack(pieces)

    def along(w):
        pieces = [w]
        for k in range(1, ranks):
            pieces.append(
                lax.ppermute(w, "sp", [(i, (i + group * k) % n_sp) for i in range(n_sp)])
            )
        return jnp.concatenate(pieces)

    all_gu = along(spread(w_gu))
    all_d = along(spread(w_d))
    if gate_weight.shape[0] % 128:
        back = (
            ((r - jnp.arange(ranks)) % ranks * group)[:, None] + (g ^ jnp.arange(group))[None, :]
        ).reshape(-1)

        def ordered(w):
            w = jnp.moveaxis(jnp.take(w, back, axis=0), 0, 2)
            return w.reshape(1, w.shape[0], w.shape[1], -1)

        all_gu = ordered(all_gu)
        all_d = ordered(all_d)
        order = jnp.zeros((1,), jnp.int32)
    else:
        order = (
            ((r - jnp.arange(ranks)) % ranks * group)[:, None] + (g ^ jnp.arange(group))[None, :]
        ).reshape(-1).astype(jnp.int32)

    folded = []
    for query, key_up in ((query_lean, key_up_lean), (query_broad, key_up_broad)):
        nope = query.shape[2] - width
        scale = query.shape[2] ** (-0.5) * LOG2E
        absorbed = jnp.einsum(
            "qhd,rhd->hqr", query[:, :, :nope], key_up, preferred_element_type=F32
        )
        turned = rotate(query[:, :, nope:].astype(F32), qpos).swapaxes(0, 1)
        folded.append((jnp.concatenate([absorbed, turned], axis=2) * scale).astype(BF))
    q = jnp.concatenate(folded)
    mixed = attention(
        jnp.reshape(r + 1, (1,)).astype(jnp.int32),
        q,
        keys,
        jnp.broadcast_to(qpos[:, None], (here, 128)),
        kpos,
        own,
        rank,
    )
    heads = query_lean.shape[1]
    term = jnp.zeros((here, out_lean.shape[2]), F32)
    for part, value_up, weight in (
        (mixed[:heads], value_up_lean, out_lean),
        (mixed[heads:], value_up_broad, out_broad),
    ):
        attended = jnp.einsum("hqr,rhv->qhv", part, value_up, preferred_element_type=F32).astype(BF)
        term = term + jnp.einsum("qhv,hvd->qd", attended, weight, preferred_element_type=F32)
    term = term.astype(BF)
    head_sum = cut(term, t, share).astype(F32)
    for k in range(1, n_tp):
        head_sum = head_sum + over_tp(cut(term, (t + k) % n_tp, share), k).astype(F32)
    branch = normalize(head_sum, attn_gain)
    kept = (residual_in.astype(F32) + branch).astype(BF)
    normed = normalize(kept.astype(F32), mlp_gain).astype(BF)

    near = jnp.stack([normed] + [over_group(normed, j) for j in range(1, group)])
    rows = jnp.stack([near] + [over_tp(near, k) for k in range(1, n_tp)])
    out = ffn(order, rows.reshape(n_tp * group * share, -1), all_gu, all_d)
    out = out.reshape(n_tp, group, share, -1)
    partial = out[0].astype(F32)
    for k in range(1, n_tp):
        partial = partial + over_tp(out[k], -k).astype(F32)
    channel_sum = partial[0]
    sent = partial.astype(BF)
    for j in range(1, group):
        channel_sum = channel_sum + over_group(sent[j], j).astype(F32)
    return (kept.astype(F32) + 0.5 * channel_sum).astype(BF)


def solution(mesh):
    in_specs = (
        P(("sp", "tp"), None),
        P("sp", "tp", None),
        P("sp", "tp", None),
        P("sp", None),
        P("sp", None),
        P(),
        P(None, "tp", None),
        P(None, "tp", None),
        P(None, "tp", None),
        P(None, "tp", None),
        P("tp", None, None),
        P("tp", None, None),
        P(),
        P(),
        P("sp", "tp"),
        P("sp", "tp"),
        P("tp", "sp"),
    )
    out_specs = P(("sp", "tp"), None)
    return jax.shard_map(shards, mesh=mesh, in_specs=in_specs, out_specs=out_specs, check_vma=False)
```
